32 devices in a mesh: sp: 8 (over z, x), tp: 4 (over y, core).
Axes of the slice: x: 2, y: 2, z: 4, core: 2. Of those that a mesh axis runs over, the one named last changes fastest.
Arguments:
- residual: bfloat16 [6144, 4096], P('sp', 'tp'), may hold values from -40 to 40
- values: bfloat16 [6144, 2048], P('sp', 'tp'), may hold values from -6 to 6
- forget_onward: bfloat16 [6144, 2048], P('sp', 'tp'), may hold values from -5.5 to 5.5
- forget_reverse: bfloat16 [6144, 2048], P('sp', 'tp'), may hold values from -5.5 to 5.5
- surge_log_decay: float32 [6144, 16], P('sp', 'tp'), may hold values from -2.1 to 0
- gate_limit_complement: float32 [2, 2048], P(None, 'tp'), may hold values from 4.8828125e-05 to 0.1
- readout_query: bfloat16 [6144, 2048], P('sp', 'tp'), may hold values from -6 to 6
- output_gate: bfloat16 [6144, 2048], P('sp', 'tp'), may hold values from -6 to 6
- head_norm_gain: float32 [128], replicated, may hold values from 0.1 to 1.9
- output_weight: bfloat16 [2048, 4096], P('tp'), may hold values from -0.125 to 0.125
- mixer_norm_gain: float32 [4096], replicated, may hold values from 0.1 to 1.9
- up_weight: bfloat16 [4096, 8192], P('sp', 'tp'), may hold values from -0.09375 to 0.09375
- down_weight: bfloat16 [4096, 8192], P('sp', 'tp'), may hold values from -0.0625 to 0.0625
Outputs:
- output: bfloat16 [6144, 4096], P('sp', 'tp')
The draws below stay inside these ranges and needn't reach their ends.
All inputs are finite; a program needn't handle non-finite values.
Results may differ from the reference program's by a relative error of at most 0.015.
Values may be sent and summed in bfloat16 or wider, within the bound.
A program may use at most 192 MiB of HBM per device.

```python
import math
import jax
import jax.numpy as jnp
from jax import lax

D = 4096
HEADS = 16
HEAD_DIM = 128
HGW = 2048
FF = 8192
TOK_DEV = 768
TOKENS = 6144
N_TP = 4


def draw_residual(key, part):
    key_one, key_two, key_three = jax.random.split(jax.random.fold_in(key, 11), 3)
    columns = jnp.arange(D, dtype=jnp.float32) / D
    col_power = 0.5 * columns + 0.5 * jax.random.uniform(key_one, (D,), jnp.float32) - 0.5
    row_power = jax.random.uniform(key_two, (TOKENS, 1), jnp.float32) - 0.5
    base_draw = jax.random.truncated_normal(key_three, -4.0, 4.0, (TOKENS, D), jnp.float32)
    return (base_draw * 10.0 ** (col_power[None, :] + row_power)).astype(jnp.bfloat16)


def forget_draw(key, salt):
    key_one, key_two = jax.random.split(jax.random.fold_in(key, salt))
    shards = TOKENS // TOK_DEV
    offset = jax.random.uniform(key_one, (shards, 1), jnp.float32, minval=-1.5, maxval=1.5)
    offset = jnp.repeat(offset, TOK_DEV, axis=0, total_repeat_length=TOKENS)
    base_draw = jax.random.truncated_normal(key_two, -4.0, 4.0, (TOKENS, HGW), jnp.float32)
    return (base_draw + offset).astype(jnp.bfloat16)


def draw_forget_onward(key, part):
    return forget_draw(key, 41)


def draw_forget_reverse(key, part):
    return forget_draw(key, 43)


def draw_gate_limit_complement(key, part):
    key_one, key_two, key_three = jax.random.split(jax.random.fold_in(key, 23), 3)
    slow_share = 0.5
    slow_heads = jax.random.uniform(key_one, (2, HEADS, 1), jnp.float32) < slow_share
    slow_gap = jnp.exp(jax.random.uniform(key_two, (2, HEADS, HEAD_DIM), jnp.float32, minval=math.log(0.3), maxval=math.log(1.5))) / TOKENS
    fast_gap = jnp.exp(jax.random.uniform(key_three, (2, HEADS, HEAD_DIM), jnp.float32, minval=math.log(0.04), maxval=math.log(0.1)))
    return jnp.where(slow_heads, slow_gap, fast_gap).reshape(2, HEADS * HEAD_DIM)


def draw_surge_log_decay(key, part):
    key_one, key_two = jax.random.split(jax.random.fold_in(key, 31))
    where_at = jax.random.randint(key_one, (3, HEADS), 0, TOKENS)
    strength = jax.random.uniform(key_two, (3, HEADS), jnp.float32, minval=math.log(0.5), maxval=math.log(0.8))
    positions = jnp.arange(TOKENS)[:, None]
    total = jnp.zeros((TOKENS, HEADS), jnp.float32)
    for turn_index in range(3):
        total = total + jnp.where(positions == where_at[turn_index][None, :], strength[turn_index][None, :], 0.0)
    return total


def block_levels(key, extent, cuts, least, high):
    loudness, own = 1.0, jax.random.fold_in(key, 6)
    for dim, parts in cuts:
        heights = jnp.exp(jax.random.uniform(jax.random.fold_in(own, dim), (parts,), jnp.float32, least / len(cuts), high / len(cuts)))
        loudness = loudness * jnp.repeat(heights, extent[dim] // parts).reshape([-1 if axis == dim else 1 for axis in range(len(extent))])
    return loudness


def centred(key, extent, spread, reach, cuts=(), kind=jnp.bfloat16):
    gain = block_levels(key, extent, cuts, -0.22, 0.18) if cuts else 1.0
    values = jax.random.normal(key, extent, jnp.float32) * spread * gain
    return jnp.minimum(jnp.maximum(values, -reach), reach).astype(kind)


def setup_inputs(seed: int = 0) -> dict:
    streams_of = jax.random.split(jax.random.key(seed), 14)
    return {
        "residual": draw_residual(jax.random.fold_in(streams_of[13], 71), 0),
        "values": centred(streams_of[1], (TOKENS, HGW), 1.0, 6.0, ((0, 8), (1, 4))),
        "forget_onward": draw_forget_onward(jax.random.fold_in(streams_of[13], 71), 0),
        "forget_reverse": draw_forget_reverse(jax.random.fold_in(streams_of[13], 71), 0),
        "surge_log_decay": draw_surge_log_decay(jax.random.fold_in(streams_of[13], 71), 0),
        "gate_limit_complement": draw_gate_limit_complement(jax.random.fold_in(streams_of[13], 71), 0),
        "readout_query": centred(streams_of[6], (TOKENS, HGW), 1.0, 6.0, ((0, 8), (1, 4))),
        "output_gate": centred(streams_of[7], (TOKENS, HGW), 1.0, 6.0, ((0, 8), (1, 4))),
        "head_norm_gain": jnp.clip(1.0 + 0.18 * jax.random.normal(streams_of[8], (HEAD_DIM,), jnp.float32), 0.1, 1.9),
        "output_weight": centred(streams_of[9], (HGW, D), HGW ** -0.5, 0.125, ((0, 4),)),
        "mixer_norm_gain": jnp.clip(1.0 + 0.18 * jax.random.normal(streams_of[10], (D,), jnp.float32), 0.1, 1.9),
        "up_weight": centred(streams_of[11], (D, FF), D ** -0.5, 0.09375, ((0, 8), (1, 4))),
        "down_weight": centred(streams_of[12], (D, FF), FF ** -0.5, 0.0625, ((0, 8), (1, 4))),
    }


epsilon = 1e-06
top_precision = lax.Precision.HIGHEST

def forget_gate_value(gate_logits, gate_lower_limit, surge_decay, head_layout):
    key_gate_random = gate_lower_limit[None, :] * jax.nn.sigmoid(-gate_logits.astype(jnp.float32))
    logarithm_decay = jnp.log1p(-key_gate_random).reshape(head_layout) + surge_decay
    return (key_gate_random.reshape(head_layout), logarithm_decay)

def sweep(queries, key_gate_random, value_rows, logarithm_decay):

    def advance(memory_state, item):
        query_at_step, key_t, value_t, decay_t = item
        memory_state = jnp.exp(decay_t)[:, :, None] * memory_state + key_t[:, :, None] * value_t[:, None, :]
        return (memory_state, jnp.einsum('mw,mwp->mp', query_at_step, memory_state, precision=top_precision))
    initial = jnp.zeros((HEADS, HEAD_DIM, HEAD_DIM), jnp.float32)
    _, outputs = lax.scan(advance, initial, (queries, key_gate_random, value_rows, logarithm_decay))
    return outputs

def grouped_sum(left, right, right_axis):
    span = left.shape[1] // N_TP
    total = jnp.zeros((left.shape[0], right.shape[1 - right_axis]), jnp.float32)
    for group in range(N_TP):
        piece = left[:, group * span:(group + 1) * span]
        if right_axis == 0:
            weight = right[group * span:(group + 1) * span]
            dims = (((1,), (0,)), ((), ()))
        else:
            weight = right[:, group * span:(group + 1) * span]
            dims = (((1,), (1,)), ((), ()))
        term = lax.dot_general(piece, weight, dims, preferred_element_type=jnp.float32)
        total = total + lax.optimization_barrier(term.astype(jnp.bfloat16)).astype(jnp.float32)
    return total

def reference(residual, values, forget_onward, forget_reverse, surge_log_decay, gate_limit_complement, readout_query, output_gate, head_norm_gain, output_weight, mixer_norm_gain, up_weight, down_weight):
    tokens = residual.shape[0]
    head_layout = (tokens, HEADS, HEAD_DIM)
    queries = (jax.nn.silu(readout_query.astype(jnp.float32)) * HEAD_DIM ** (-0.5)).reshape(head_layout)
    value_rows = values.astype(jnp.float32).reshape(head_layout)
    surge_decay = surge_log_decay[:, :, None]
    key_onward, logarithm_onward = forget_gate_value(forget_onward, gate_limit_complement[0], surge_decay, head_layout)
    key_reverse, logarithm_reverse = forget_gate_value(forget_reverse, gate_limit_complement[1], surge_decay, head_layout)
    forward = sweep(queries, key_onward, value_rows, logarithm_onward)
    backward = jnp.flip(sweep(jnp.flip(queries, 0), jnp.flip(key_reverse, 0), jnp.flip(value_rows, 0), jnp.flip(logarithm_reverse, 0)), 0)
    mixed_out = forward + backward
    normed = mixed_out * lax.rsqrt(lax.optimization_barrier(jnp.mean(mixed_out * mixed_out, axis=-1, keepdims=True)) + epsilon) * head_norm_gain
    gated_rows = (normed.reshape(tokens, HEADS * HEAD_DIM) * jax.nn.silu(output_gate.astype(jnp.float32))).astype(jnp.bfloat16)
    attention = grouped_sum(gated_rows, output_weight, 0)
    middle = (residual.astype(jnp.float32) + attention).astype(jnp.bfloat16)
    middle_f = middle.astype(jnp.float32)
    scale_rows = lax.rsqrt(lax.optimization_barrier(jnp.mean(middle_f * middle_f, axis=1, keepdims=True)) + epsilon)
    normalized = (middle_f * scale_rows * mixer_norm_gain).astype(jnp.bfloat16)
    lifted = jnp.dot(normalized, up_weight, preferred_element_type=jnp.float32)
    hidden = jnp.square(jax.nn.relu(lifted)).astype(jnp.bfloat16)
    channel = grouped_sum(hidden, down_weight, 1)
    return (middle_f + channel).astype(jnp.bfloat16)
```

```python
import jax
import jax.numpy as jnp
from jax import lax
from jax.experimental import pallas as pl
from jax.experimental.pallas import tpu as pltpu
from jax.sharding import PartitionSpec as P

HEAD_DIM = 128
CHUNK = 128


epsilon = 1e-06
f32 = jnp.float32
bf16 = jnp.bfloat16

NT = (((1,), (1,)), ((), ()))
TN = (((0,), (0,)), ((), ()))


def dot(a, b, dims=(((1,), (0,)), ((), ()))):
    return lax.dot_general(a, b, dims, preferred_element_type=f32)


def running_sum(triangle, x):
    high = x.astype(bf16)
    low = (x - high.astype(f32)).astype(bf16)
    return dot(triangle, high) + dot(triangle, low)


def recurrence_kernel(
    query_ref, value_ref, fwd_ref, bwd_ref, surge_ref, limit_ref,
    mixed_ref, qf_ref, qb_ref, state_ref, decay_ref,
):
    rows = query_ref.shape[0]
    chunks = rows // CHUNK
    at = lax.broadcasted_iota(jnp.int32, (CHUNK, CHUNK), 0)
    src = lax.broadcasted_iota(jnp.int32, (CHUNK, CHUNK), 1)
    for way, (gate_ref, q_ref) in enumerate(((fwd_ref, qf_ref), (bwd_ref, qb_ref))):
        seen = src <= at if way == 0 else src >= at
        triangle = jnp.where(seen, 1.0, 0.0).astype(bf16)
        limit = limit_ref[way : way + 1, :]
        state = jnp.zeros((HEAD_DIM, HEAD_DIM), f32)
        before = jnp.zeros((1, HEAD_DIM), f32)
        last = CHUNK - 1 if way == 0 else 0
        for step in range(chunks):
            n = step if way == 0 else chunks - 1 - step
            span = pl.ds(n * CHUNK, CHUNK)
            query = query_ref[span, :].astype(f32)
            query = query * jax.nn.sigmoid(query) * HEAD_DIM ** (-0.5)
            value = value_ref[span, :]
            key = limit * jax.nn.sigmoid(-gate_ref[span, :].astype(f32))
            gate = running_sum(triangle, jnp.log1p(-key))
            surge = running_sum(triangle, surge_ref[span, :])
            gate_end, surge_end = gate[last : last + 1], surge[last : last + 1]
            query_gate = query * jnp.exp(gate)
            key_rise = key * jnp.exp(-gate)
            scores = dot(query_gate.astype(bf16), key_rise.astype(bf16), NT)
            scores = scores * jnp.where(seen, jnp.exp(surge - surge.T), 0.0)
            out = dot(scores.astype(bf16), value)
            query_decay = query_gate * jnp.exp(surge)
            if step > 0:
                out = out + dot(query_decay.astype(bf16), state.astype(bf16), NT)
            if way == 0:
                mixed_ref[span, :] = out
            else:
                mixed_ref[span, :] += out
            q_ref[span, :] = (query_decay * jnp.exp(before)).astype(bf16)
            key_tail = key * jnp.exp((gate_end - gate) + (surge_end - surge))
            whole = gate_end + surge_end
            state = state * jnp.exp(whole) + dot(value, key_tail.astype(bf16), TN)
            before = before + whole
        state_ref[way, 0] = state.astype(bf16)
        decay_ref[0, way : way + 1, :] = before


def recurrence(query, value, fwd, bwd, surge, limit):
    rows, channels = query.shape
    heads = channels // HEAD_DIM
    tall = pl.BlockSpec((rows, HEAD_DIM), lambda h: (0, h))
    return pl.pallas_call(
        recurrence_kernel,
        grid=(heads,),
        in_specs=[tall] * 5 + [pl.BlockSpec((2, HEAD_DIM), lambda h: (0, h))],
        out_specs=[
            tall,
            tall,
            tall,
            pl.BlockSpec((2, 1, HEAD_DIM, HEAD_DIM), lambda h: (0, h, 0, 0)),
            pl.BlockSpec((1, 2, HEAD_DIM), lambda h: (h, 0, 0)),
        ],
        out_shape=[
            jax.ShapeDtypeStruct((rows, channels), f32),
            jax.ShapeDtypeStruct((rows, channels), bf16),
            jax.ShapeDtypeStruct((rows, channels), bf16),
            jax.ShapeDtypeStruct((2, heads, HEAD_DIM, HEAD_DIM), bf16),
            jax.ShapeDtypeStruct((heads, 2, HEAD_DIM), f32),
        ],
        cost_estimate=pl.CostEstimate(
            flops=40 * rows * channels * HEAD_DIM,
            bytes_accessed=20 * rows * channels,
            transcendentals=20 * rows * channels,
        ),
        name="recurrence",
    )(query, value, fwd, bwd, surge, limit)


def finish_kernel(mixed_ref, qf_ref, qb_ref, state_ref, gain_ref, gate_ref, out_ref):
    mixed = mixed_ref[...]
    mixed = mixed + dot(qf_ref[...], state_ref[0, 0], NT) + dot(qb_ref[...], state_ref[1, 0], NT)
    scale = lax.rsqrt(jnp.mean(mixed * mixed, axis=-1, keepdims=True) + epsilon)
    gate = gate_ref[...].astype(f32)
    out = mixed * scale * gain_ref[...] * (gate * jax.nn.sigmoid(gate))
    out_ref[...] = out.astype(bf16)


def finish(mixed, qf, qb, states, gain, gate):
    rows, channels = mixed.shape
    heads = channels // HEAD_DIM
    tall = pl.BlockSpec((rows, HEAD_DIM), lambda h: (0, h))
    return pl.pallas_call(
        finish_kernel,
        grid=(heads,),
        in_specs=[
            tall,
            tall,
            tall,
            pl.BlockSpec((2, 1, HEAD_DIM, HEAD_DIM), lambda h: (0, h, 0, 0)),
            pl.BlockSpec((1, HEAD_DIM), lambda h: (0, 0)),
            tall,
        ],
        out_specs=tall,
        out_shape=jax.ShapeDtypeStruct((rows, channels), bf16),
        cost_estimate=pl.CostEstimate(
            flops=4 * rows * channels * HEAD_DIM,
            bytes_accessed=12 * rows * channels,
            transcendentals=2 * rows * channels,
        ),
        name="finish",
    )(mixed, qf, qb, states, gain, gate)


def incoming(states, decays):
    devices, me = lax.axis_size("sp"), lax.axis_index("sp")
    states = lax.all_gather(states, "sp")
    decays = lax.all_gather(decays, "sp")
    origin = jnp.arange(devices)[:, None]
    between = jnp.arange(devices)[None, :]
    result = []
    for way in range(2):
        if way == 0:
            reached, inside = origin < me, (between > origin) & (between < me)
        else:
            reached, inside = origin > me, (between < origin) & (between > me)
        log_weight = jnp.sum(
            jnp.where(inside[:, :, None, None], decays[None, :, :, way, :], 0.0), axis=1
        )
        weight = jnp.where(reached[:, :, None], jnp.exp(log_weight), 0.0)
        result.append(jnp.sum(weight[:, :, None, :] * states[:, way].astype(f32), axis=0))
    return jnp.stack(result).astype(bf16)


def spread(block):
    devices, me = lax.axis_size("sp"), lax.axis_index("sp")

    def shift(value, by):
        return lax.ppermute(value, "sp", [(i, (i + by) % devices) for i in range(devices)])

    if devices != 8:
        return [(block, me)] + [
            (shift(block, by), (me + devices - by) % devices) for by in range(1, devices)
        ]

    def flip(value):
        return lax.ppermute(value, "sp", [(i, i ^ 1) for i in range(devices)])

    half = block.shape[0] // 2
    side = flip(block)
    low, high = shift(block, 2), shift(block, -2)
    low_side, high_side = shift(side, 2), shift(side, -2)
    far_top, far_bottom = shift(low[:half], 2), shift(high[half:], -2)
    far = jnp.concatenate([far_top, far_bottom], axis=0)
    far_side = jnp.concatenate([flip(far_top), flip(far_bottom)], axis=0)
    partner = me + 1 - 2 * (me % 2)
    return [
        (block, me),
        (side, partner),
        (low, (me + 6) % 8),
        (high, (me + 2) % 8),
        (low_side, (partner + 6) % 8),
        (high_side, (partner + 2) % 8),
        (far, (me + 4) % 8),
        (far_side, (partner + 4) % 8),
    ]


def per_device(
    residual,
    values,
    forget_onward,
    forget_reverse,
    surge_log_decay,
    gate_limit_complement,
    readout_query,
    output_gate,
    head_norm_gain,
    output_weight,
    mixer_norm_gain,
    up_weight,
    down_weight,
):
    rows, channels = values.shape
    up_blocks, down_blocks = spread(up_weight), spread(down_weight)
    span = up_weight.shape[0]
    model = output_weight.shape[1]

    surge = jnp.repeat(surge_log_decay, HEAD_DIM, axis=1)
    mixed, qf, qb, states, decays = recurrence(
        readout_query, values, forget_onward, forget_reverse, surge, gate_limit_complement
    )
    states = incoming(states, decays)
    gated = finish(mixed, qf, qb, states, head_norm_gain[None, :], output_gate)

    partial_value = dot(gated, output_weight)
    attention = lax.psum_scatter(
        partial_value.astype(bf16), "tp", scatter_dimension=1, tiled=True
    ).astype(f32)
    middle = (residual.astype(f32) + attention).astype(bf16).astype(f32)
    squares = lax.psum(jnp.sum(middle * middle, axis=1), "tp")
    own_cols = middle.shape[1]
    gain_part = lax.dynamic_slice_in_dim(mixer_norm_gain, lax.axis_index("tp") * own_cols, own_cols)
    scale_rows = lax.rsqrt(squares / model + epsilon)[:, None]
    normalized = (middle * scale_rows * gain_part).astype(bf16)
    normalized = lax.all_gather(normalized, "tp", axis=1, tiled=True)

    up_full = jnp.zeros((model, up_weight.shape[1]), bf16)
    for block, owner in up_blocks:
        up_full = lax.dynamic_update_slice(up_full, block, (owner * span, 0))
    hidden = jnp.square(jax.nn.relu(dot(normalized, up_full))).astype(bf16)
    channel_part = jnp.zeros((rows, model), bf16)
    for block, owner in down_blocks:
        piece = dot(hidden, block, NT).astype(bf16)
        channel_part = lax.dynamic_update_slice(channel_part, piece, (0, owner * span))
    channel = lax.psum_scatter(channel_part, "tp", scatter_dimension=1, tiled=True)
    return (middle + channel.astype(f32)).astype(bf16)


def solution(mesh):
    placed = (
        P("sp", "tp"),
        P("sp", "tp"),
        P("sp", "tp"),
        P("sp", "tp"),
        P("sp", "tp"),
        P(None, "tp"),
        P("sp", "tp"),
        P("sp", "tp"),
        P(),
        P("tp", None),
        P(),
        P("sp", "tp"),
        P("sp", "tp"),
    )
    return jax.shard_map(
        per_device, mesh=mesh, in_specs=placed, out_specs=P("sp", "tp"), check_vma=False
    )
```
